32 devices in a mesh: ep: 8 (over z, y), tp: 4 (over x, core).
Axes of the slice: x: 2, y: 2, z: 4, core: 2. Of those that a mesh axis runs over, the one named last changes fastest.
Arguments:
- tokens: bfloat16 [6144, 2048], P('ep')
- in_gain: float32 [2048], replicated, may hold values from 0.1 to 1.9
- route_ids: int32 [6144, 2], P('ep'), may hold values from 0 to 7, all different within a row; in each aligned block of 768 rows (0 to 767, 768 to 1535, ...) at most 384 rows name the same one
- route_scores: float32 [6144, 2], P('ep'), may hold values from 0.1 to 1
- gate_weight: bfloat16 [8, 2048, 1024], P('ep', None, 'tp'), may hold values from -0.125 to 0.125
- up_weight: bfloat16 [8, 2048, 1024], P('ep', None, 'tp'), may hold values from -0.125 to 0.125
- down_weight: bfloat16 [8, 1024, 2048], P('ep', 'tp')
- out_gain: float32 [2048], P('tp'), may hold values from 0.1 to 1.9
Outputs:
- mixed: bfloat16 [6144, 2048], P('ep', 'tp')
The draws below stay inside these ranges and needn't reach their ends.
Inputs may be any that keep to these rules, and one draw needn't show every extreme that they name: `route_ids`: each row names 2 different experts. Among the rows of one index of ep (aligned blocks of 768 rows) no expert is named more than 384 times, a bound that some block reaches.
All inputs are finite; a program needn't handle non-finite values.
Results may differ from the reference program's by a relative error of at most 0.012.
Values may be sent and summed in bfloat16 or wider, within the bound.
A program may use at most 128 MiB of HBM per device.

```python
import math
import jax
import jax.numpy as jnp
import numpy as np
from jax import lax

D = 2048
FF = 1024
TOP_K = 2
TOK_DEV = 768
EXPERTS = 8
TOKENS = 6144
CAP = 384
FF_PART = 256
N_EP = 8
N_TP = 4


def draw_tokens(key, part):
    keys = jax.random.split(jax.random.fold_in(key, 3), 3)
    row_scale = 10.0 ** jax.random.uniform(keys[1], (TOKENS, 1), jnp.float32)
    column_scale = 10.0 ** (0.5 * jax.random.uniform(keys[2], (1, D), jnp.float32))
    values = jax.random.normal(keys[0], (TOKENS, D), jnp.float32) * row_scale * column_scale
    return values.astype(jnp.bfloat16)


def draw_down_weight(key, part):
    keys = jax.random.split(jax.random.fold_in(key, 11), 2)
    position = jnp.arange(D, dtype=jnp.float32) / D
    base = jax.random.normal(keys[0], (EXPERTS, FF, D), jnp.float32)
    scale = 10.0 ** (0.5 * position + 0.5 * jax.random.uniform(keys[1], (D,), jnp.float32))
    return (base * FF ** (-0.5) * scale[None, None, :]).astype(jnp.bfloat16)


def steps_of(stream_key, dims, pieces, smallest, top_value):
    loudness = 1.0
    for dim, parts in pieces:
        draws = jax.random.uniform(jax.random.fold_in(jax.random.fold_in(stream_key, 6), dim), (parts,), jnp.float32, smallest / len(pieces), top_value / len(pieces))
        loudness = loudness * jnp.repeat(jnp.exp(draws), dims[dim] // parts).reshape((-1,) + (1,) * (len(dims) - 1 - dim))
    return loudness


def routed_block(own_key, own, number, rows, count, top, reach, lean):
    sequence = jax.random.permutation(own_key, count)
    crowded, usual = shares(count, rows * top, reach, lean, True), shares(count, rows * top, reach, lean, False)
    places = jnp.arange(count)

    def named(tallies, rotation):
        used = int((tallies > 0).sum())
        fixed = max(1, used // 4)
        moved = fixed + (places - fixed + rotation * (used - fixed)) % max(1, count - fixed)
        return jnp.zeros((count,), jnp.int32).at[sequence[jnp.where(places < fixed, places, moved)]].set(jnp.asarray(tallies, jnp.int32))

    tallies = jnp.where(number % 4 == 0, named(crowded, number // 4), named(usual, number - number // 4 - 1))
    mixed = jax.random.permutation(jax.random.fold_in(own, 3), count)
    giver, sink = mixed[0:count // 2 * 2:2], mixed[1:count // 2 * 2:2]
    margin = jnp.minimum(tallies[giver] - 1, reach - tallies[sink]) // 2
    margin = jnp.where((giver == sequence[0]) | (sink == sequence[0]) | (tallies[sink] == 0), 0, jnp.maximum(margin, 0))
    moved = jax.random.randint(jax.random.fold_in(own, 4), (count // 2,), 0, 1 << 20) % (margin + 1)
    tallies = tallies.at[giver].add(-moved).at[sink].add(moved)
    labels = jnp.searchsorted(jnp.cumsum(tallies), jnp.arange(rows * top), side="right").astype(jnp.int32)
    listing = labels.reshape(top, rows).T
    listing = listing[jax.random.permutation(jax.random.fold_in(own, 1), rows)]
    rotation = jax.random.randint(jax.random.fold_in(own, 2), (rows, 1), 0, top)
    return jnp.take_along_axis(listing, (jnp.arange(top)[None, :] + rotation) % top, axis=1)


def shares(count, total, most, slope, full):
    weights = [(1 << 20) // math.isqrt(standing ** slope) + 1 for standing in range(1, count + 1)]
    largest = most if full else min(most, max(-(-total // count), total * weights[0] // sum(weights)))
    least = 1 if total - largest >= count - 1 else 0
    counts, spare = [largest] + [least] * (count - 1), total - largest - least * (count - 1)
    while spare > 0:
        candidates = [i for i in range(1, count) if counts[i] < largest] or [i for i in range(1, count) if counts[i] < most]
        pool, left = sum([weights[i] for i in candidates]), spare
        for i in candidates:
            addition = min(most - counts[i], max(1, left * weights[i] // pool), spare)
            counts[i] = counts[i] + addition
            spare = spare - addition
    return np.array(counts)


def noise(stream_key, shape, scale, most, cuts=(), kind=jnp.bfloat16):
    values = scale * jax.random.normal(stream_key, shape, jnp.float32)
    if cuts:
        values = values * steps_of(stream_key, shape, cuts, -0.22, 0.18)
    return jnp.clip(values, -most, most).astype(kind)


def setup_inputs(seed: int = 0) -> dict:
    key_of = jax.random.split(jax.random.key(seed), 9)
    tokens = draw_tokens(jax.random.fold_in(key_of[8], 71), 0)
    in_gain = jnp.clip(1.0 + 0.18 * jax.random.normal(key_of[1], (D,), jnp.float32), 0.1, 1.9)
    route_ids_keys = jax.random.split(jax.random.fold_in(key_of[2], 1), TOKENS // TOK_DEV)
    route_ids_turns = jax.random.permutation(jax.random.fold_in(key_of[2], 3), TOKENS // TOK_DEV)
    route_ids = jax.vmap(lambda own, number: routed_block(jax.random.fold_in(key_of[2], 2), own, number, TOK_DEV, EXPERTS, TOP_K, CAP, 2))(route_ids_keys, route_ids_turns).reshape((TOKENS, TOP_K))
    route_scores = jnp.clip(jnp.exp(math.log(1.0) - 2.3025851 * jax.random.uniform(key_of[3], (TOKENS, TOP_K), jnp.float32) ** steps_of(key_of[3], (TOKENS, TOP_K), ((0, 8),), -0.2, 0.2)), 0.1, 1.0)
    gate_weight = noise(key_of[4], (EXPERTS, D, FF), D ** -0.5, 0.125, ((0, 8), (2, 4)))
    up_weight = noise(key_of[5], (EXPERTS, D, FF), D ** -0.5, 0.125, ((0, 8), (2, 4)))
    down_weight = draw_down_weight(jax.random.fold_in(key_of[8], 71), 0)
    out_gain = jnp.clip(1.0 + 0.18 * jax.random.normal(key_of[7], (D,), jnp.float32), 0.1, 1.9)
    return dict(tokens=tokens, in_gain=in_gain, route_ids=route_ids, route_scores=route_scores, gate_weight=gate_weight, up_weight=up_weight, down_weight=down_weight, out_gain=out_gain)


epsilon = 1e-06

def reference(tokens, in_gain, route_ids, route_scores, gate_weight, up_weight, down_weight, out_gain):
    as_float = tokens.astype(jnp.float32)
    normed = (as_float * lax.rsqrt(lax.optimization_barrier(jnp.mean(as_float * as_float, axis=1, keepdims=True)) + epsilon) * in_gain).astype(jnp.bfloat16)
    flat_ids = route_ids.reshape(N_EP, TOK_DEV * TOP_K)
    one_hot = (flat_ids[:, :, None] == jnp.arange(EXPERTS, dtype=jnp.int32)[None, None, :]).astype(jnp.int32)
    slot_index = lax.optimization_barrier(jnp.sum((jnp.cumsum(one_hot, axis=1) - 1) * one_hot, axis=2)).astype(jnp.int32)
    block_index = jnp.broadcast_to(jnp.arange(N_EP, dtype=jnp.int32)[:, None], flat_ids.shape)
    row_index = (block_index * TOK_DEV + jnp.arange(TOK_DEV * TOP_K, dtype=jnp.int32)[None, :] // TOP_K).astype(jnp.int32)
    buffer = jnp.zeros((EXPERTS, N_EP, CAP, D), jnp.bfloat16)
    buffer = buffer.at[flat_ids, block_index, slot_index].set(normed[row_index])

    def expert_run(inputs):
        rows_in, gate_w, up_w, down_w = inputs
        gate_acts = jnp.dot(rows_in, gate_w, preferred_element_type=jnp.float32)
        up_acts = jnp.dot(rows_in, up_w, preferred_element_type=jnp.float32)
        hidden = (jax.nn.silu(gate_acts) * up_acts).astype(jnp.bfloat16)
        hidden_blocks = hidden.reshape(-1, N_TP, FF_PART).astype(jnp.float32)
        down_blocks = down_w.reshape(N_TP, FF_PART, D).astype(jnp.float32)
        partial_value = jnp.einsum('rpf,pfd->prd', hidden_blocks, down_blocks)
        rounded = lax.optimization_barrier(partial_value.astype(jnp.bfloat16))
        return lax.optimization_barrier(jnp.sum(rounded.astype(jnp.float32), axis=0)).astype(jnp.bfloat16)
    outputs = lax.map(expert_run, (buffer.reshape(EXPERTS, N_EP * CAP, D), gate_weight, up_weight, down_weight))
    outputs = outputs.reshape(EXPERTS, N_EP, CAP, D)
    picked = outputs[flat_ids, block_index, slot_index].astype(jnp.float32).reshape(TOKENS, TOP_K, D)
    mix_weight = route_scores / lax.optimization_barrier(jnp.sum(route_scores, axis=1, keepdims=True))
    combined = lax.optimization_barrier(jnp.sum(mix_weight[:, :, None] * picked, axis=1))
    mixed = combined * lax.rsqrt(lax.optimization_barrier(jnp.mean(combined * combined, axis=1, keepdims=True)) + epsilon) * out_gain
    return mixed.astype(jnp.bfloat16)
```

```python
import jax
import jax.numpy as jnp
from jax import lax
from jax.sharding import PartitionSpec as P

epsilon = 1e-06


def gathered(block, count):
    blocks = [block]
    bit = 1
    swaps = []
    while bit < count:
        swaps.append([(i, i ^ bit) for i in range(count)])
        bit *= 2
    first = lax.ppermute(block, "tp", swaps[0])
    blocks.append(first)
    for pairs in swaps[1:]:
        far = lax.ppermute(block, "tp", pairs)
        blocks.append(far)
        blocks.append(lax.ppermute(far, "tp", swaps[0]))
    return blocks


def per_device(
    tokens, in_gain, route_ids, route_scores, gate_weight, up_weight, down_weight, out_gain
):
    count_ep = lax.axis_size("ep")
    count_tp = lax.axis_size("tp")
    experts = count_ep * gate_weight.shape[0]
    tok_count, full_width = tokens.shape
    rows = tok_count // count_tp
    start = lax.axis_index("tp") * rows
    gates = gathered(gate_weight[0], count_tp)
    ups = gathered(up_weight[0], count_tp)
    downs = gathered(down_weight[0], count_tp)
    gain_full = lax.all_gather(out_gain, "tp", axis=0, tiled=True)

    as_float = lax.dynamic_slice_in_dim(tokens, start, rows, 0).astype(jnp.float32)
    normed = (
        as_float
        * lax.rsqrt(jnp.mean(as_float * as_float, axis=1, keepdims=True) + epsilon)
        * in_gain
    ).astype(jnp.bfloat16)
    spread = lax.all_gather(normed, "ep", axis=0, tiled=True)

    ids = lax.dynamic_slice_in_dim(route_ids, start, rows, 0)
    scores = lax.dynamic_slice_in_dim(route_scores, start, rows, 0)
    mix = scores / jnp.sum(scores, axis=1, keepdims=True)
    chosen = ids[:, :, None] == jnp.arange(experts, dtype=jnp.int32)[None, None, :]
    dense = jnp.sum(jnp.where(chosen, mix[:, :, None], 0.0), axis=1).T
    weight = lax.all_to_all(dense, "ep", split_axis=0, concat_axis=0, tiled=True).reshape(-1, 1)

    def hidden_of(gate_w, up_w):
        gate_acts = jnp.dot(spread, gate_w, preferred_element_type=jnp.float32)
        up_acts = jnp.dot(spread, up_w, preferred_element_type=jnp.float32)
        return (jax.nn.silu(gate_acts) * up_acts).astype(jnp.bfloat16)

    hidden = jnp.concatenate(
        [
            hidden_of(jnp.concatenate(gates[i : i + 2], 1), jnp.concatenate(ups[i : i + 2], 1))
            for i in range(0, count_tp, 2)
        ],
        1,
    )
    expert_out = jnp.dot(
        hidden, jnp.concatenate(downs, 0), preferred_element_type=jnp.float32
    )
    terms = jnp.where(weight > 0.0, weight * expert_out, 0.0).astype(jnp.bfloat16)
    combined = lax.psum_scatter(terms, "ep", scatter_dimension=0, tiled=True).astype(jnp.float32)
    scale = lax.rsqrt(jnp.mean(combined * combined, axis=1, keepdims=True) + epsilon)
    mixed = (combined * scale * gain_full).astype(jnp.bfloat16)
    return lax.all_to_all(mixed, "tp", split_axis=1, concat_axis=0, tiled=True)


def solution(mesh):
    in_specs = (
        P("ep", None),
        P(),
        P("ep", None),
        P("ep", None),
        P("ep", None, "tp"),
        P("ep", None, "tp"),
        P("ep", "tp", None),
        P("tp"),
    )
    out_specs = P("ep", "tp")
    return jax.shard_map(
        per_device, mesh=mesh, in_specs=in_specs, out_specs=out_specs, check_vma=False
    )
```

```python
import jax
import jax.numpy as jnp
from jax import lax
from jax.sharding import PartitionSpec as P

epsilon = 1e-06


def gathered(block, count):
    blocks = [block]
    bit = 1
    swaps = []
    while bit < count:
        swaps.append([(i, i ^ bit) for i in range(count)])
        bit *= 2
    first = lax.ppermute(block, "tp", swaps[0])
    blocks.append(first)
    for pairs in swaps[1:]:
        far = lax.ppermute(block, "tp", pairs)
        blocks.append(far)
        blocks.append(lax.ppermute(far, "tp", swaps[0]))
    return blocks


def per_device(
    tokens, in_gain, route_ids, route_scores, gate_weight, up_weight, down_weight, out_gain
):
    count_ep = lax.axis_size("ep")
    count_tp = lax.axis_size("tp")
    experts = count_ep * gate_weight.shape[0]
    tok_count, full_width = tokens.shape
    rows = tok_count // count_tp
    start = lax.axis_index("tp") * rows
    gates = gathered(gate_weight[0], count_tp)
    ups = gathered(up_weight[0], count_tp)
    downs = gathered(down_weight[0], count_tp)
    gain_full = lax.all_gather(out_gain, "tp", axis=0, tiled=True)

    as_float = lax.dynamic_slice_in_dim(tokens, start, rows, 0).astype(jnp.float32)
    normed = (
        as_float
        * lax.rsqrt(jnp.mean(as_float * as_float, axis=1, keepdims=True) + epsilon)
        * in_gain
    ).astype(jnp.bfloat16)
    ring = count_ep // 2
    pair_swap = [(i, i ^ 1) for i in range(count_ep)]
    ring_step = [(i, (i + 2) % count_ep) for i in range(count_ep)]
    held = [normed]
    for _ in range(1, ring):
        held.append(lax.ppermute(held[-1], "ep", ring_step))
    partner = [lax.ppermute(block, "ep", pair_swap) for block in held]

    ids = lax.dynamic_slice_in_dim(route_ids, start, rows, 0)
    scores = lax.dynamic_slice_in_dim(route_scores, start, rows, 0)
    mix = scores / jnp.sum(scores, axis=1, keepdims=True)
    chosen = ids[:, :, None] == jnp.arange(experts, dtype=jnp.int32)[None, None, :]
    dense = jnp.sum(jnp.where(chosen, mix[:, :, None], 0.0), axis=1).T
    weight = lax.all_to_all(dense, "ep", split_axis=0, concat_axis=0, tiled=True).reshape(count_ep, rows)

    gates, ups, held = lax.optimization_barrier((gates, ups, held))
    gate_full = jnp.concatenate(gates, 1)
    up_full = jnp.concatenate(ups, 1)
    down_full = jnp.concatenate(downs, 0)
    me = lax.axis_index("ep")

    def terms_of(step):
        block = jnp.concatenate([held[step], partner[step]], 0)
        gate_acts = jnp.dot(block, gate_full, preferred_element_type=jnp.float32)
        up_acts = jnp.dot(block, up_full, preferred_element_type=jnp.float32)
        hidden = (jax.nn.silu(gate_acts) * up_acts).astype(jnp.bfloat16)
        expert_out = jnp.dot(hidden, down_full, preferred_element_type=jnp.float32)
        source = (me + count_ep - 2 * step) % count_ep
        share = jnp.concatenate(
            [
                lax.dynamic_index_in_dim(weight, source, 0, keepdims=False),
                lax.dynamic_index_in_dim(weight, source ^ 1, 0, keepdims=False),
            ]
        )[:, None]
        terms = jnp.where(share > 0.0, share * expert_out, 0.0).astype(jnp.bfloat16)
        return terms[:rows], terms[rows:]

    running = None
    for step in list(range(1, ring)) + [0]:
        own, other = terms_of(step)
        total = own.astype(jnp.float32) + lax.ppermute(other, "ep", pair_swap).astype(jnp.float32)
        if running is not None:
            total = total + lax.ppermute(running, "ep", ring_step).astype(jnp.float32)
        running = total.astype(jnp.bfloat16)
    combined = total
    scale = lax.rsqrt(jnp.mean(combined * combined, axis=1, keepdims=True) + epsilon)
    mixed = (combined * scale * gain_full).astype(jnp.bfloat16)
    return lax.all_to_all(mixed, "tp", split_axis=1, concat_axis=0, tiled=True)


def solution(mesh):
    in_specs = (
        P("ep", None),
        P(),
        P("ep", None),
        P("ep", None),
        P("ep", None, "tp"),
        P("ep", None, "tp"),
        P("ep", "tp", None),
        P("tp"),
    )
    out_specs = P("ep", "tp")
    return jax.shard_map(
        per_device, mesh=mesh, in_specs=in_specs, out_specs=out_specs, check_vma=False
    )
```
